32 devices in a mesh: ep: 8 (over z, y), tp: 4 (over x, core).
Axes of the slice: x: 2, y: 2, z: 4, core: 2. Of those that a mesh axis runs over, the one named last changes fastest.
Arguments:
- tokens: bfloat16 [2048, 2048], P('ep', 'tp'), may hold values from -72 to 72
- norm_gain: bfloat16 [2048], P('tp'), may hold values from 0.099609375 to 1.8984375
- expert_ids: int32 [2048, 2], P('ep'), may hold values from 0 to 7, all different within a row; in each aligned block of 256 rows (0 to 255, 256 to 511, ...) at most 128 rows name the same one
- gate_share: float32 [2048, 2], P('ep'), may hold values from 0.1 to 1
- gate_weight: bfloat16 [8, 2048, 4096], P('ep', None, 'tp'), may hold values from -0.125 to 0.125
- up_weight: bfloat16 [8, 2048, 4096], P('ep', None, 'tp'), may hold values from -0.125 to 0.125
- down_weight: bfloat16 [8, 4096, 2048], P('ep', 'tp'), may hold values from -0.09375 to 0.09375
Outputs:
- mixed: bfloat16 [2048, 2048], P('ep', 'tp')
The draws below stay inside these ranges and needn't reach their ends.
Inputs may be any that keep to these rules, and one draw needn't show every extreme that they name: `expert_ids`: each token names two different experts; among the 256 tokens of one index of ep no expert is named more than 128 times, a bound that some block reaches.
All inputs are finite; a program needn't handle non-finite values.
Results may differ from the reference program's by a relative error of at most 0.019.
Values may be sent and summed in bfloat16 or wider, within the bound.
A program may use at most 64 MiB of HBM per device.

```python
import math
import jax
import jax.numpy as jnp
import numpy as np
from jax import lax

D = 2048
FF = 4096
TOK_DEV = 256
EXPERTS = 8
CAP = 128
TOKENS = 2048
N_EP = 8
N_TP = 4


def draw_tokens(key, part):
    first, second, third = jax.random.split(key, 3)
    scales = jnp.exp(jax.random.uniform(second, (N_TP,), jnp.float32, jnp.log(0.3), jnp.log(3.0)))
    columns = jnp.repeat(scales, D // N_TP)
    base = jnp.clip(jax.random.normal(first, (TOKENS, D), jnp.float32), -6.0, 6.0)
    return (base * columns[None, :]).astype(jnp.bfloat16)


def levels(rng, extent, pieces, smallest, high):
    def one(dim, shards_of):
        draws = jax.random.uniform(jax.random.fold_in(jax.random.fold_in(rng, 6), dim), (shards_of,), jnp.float32, smallest / len(pieces), high / len(pieces))
        return jnp.repeat(jnp.exp(draws), extent[dim] // shards_of).reshape((-1,) + (1,) * (len(extent) - dim - 1))

    factor_of = one(*pieces[0])
    for cut in pieces[1:]:
        factor_of = factor_of * one(*cut)
    return factor_of


def routed_block(own_key, own, number, rows, count, top, most, skew):
    ranking = jax.random.permutation(own_key, count)
    packed, common = portions_of(count, rows * top, most, skew, True), portions_of(count, rows * top, most, skew, False)
    places = jnp.arange(count)

    def named(lengths, turn):
        used = int((lengths > 0).sum())
        fixed = max(1, used // 4)
        passed = fixed + (places - fixed + turn * (used - fixed)) % max(1, count - fixed)
        return jnp.zeros((count,), jnp.int32).at[ranking[jnp.where(places < fixed, places, passed)]].set(jnp.asarray(lengths, jnp.int32))

    lengths = jnp.where(number % 4 == 0, named(packed, number // 4), named(common, number - number // 4 - 1))
    mixed = jax.random.permutation(jax.random.fold_in(own, 3), count)
    source_of, sink = mixed[0:count // 2 * 2:2], mixed[1:count // 2 * 2:2]
    slack = jnp.minimum(lengths[source_of] - 1, most - lengths[sink]) // 2
    slack = jnp.where((source_of == ranking[0]) | (sink == ranking[0]) | (lengths[sink] == 0), 0, jnp.maximum(slack, 0))
    passed = jax.random.randint(jax.random.fold_in(own, 4), (count // 2,), 0, 1 << 20) % (slack + 1)
    lengths = lengths.at[source_of].add(-passed).at[sink].add(passed)
    members = jnp.searchsorted(jnp.cumsum(lengths), jnp.arange(rows * top), side="right").astype(jnp.int32)
    table = members.reshape(top, rows).T
    table = table[jax.random.permutation(jax.random.fold_in(own, 1), rows)]
    turn = jax.random.randint(jax.random.fold_in(own, 2), (rows, 1), 0, top)
    return jnp.take_along_axis(table, (jnp.arange(top)[None, :] + turn) % top, axis=1)


def portions_of(count, total, limit, skew, full):
    loads = [(1 << 20) // math.isqrt(standing ** skew) + 1 for standing in range(1, count + 1)]
    largest = limit if full else min(limit, max(-(-total // count), total * loads[0] // sum(loads)))
    least = 1 if total - largest >= count - 1 else 0
    given, spare = [largest] + [least] * (count - 1), total - largest - least * (count - 1)
    while spare > 0:
        free = [i for i in range(1, count) if given[i] < largest] or [i for i in range(1, count) if given[i] < limit]
        mass, remaining = sum([loads[i] for i in free]), spare
        for i in free:
            addition = min(limit - given[i], max(1, remaining * loads[i] // mass), spare)
            given[i] = given[i] + addition
            spare = spare - addition
    return np.array(given)


def normal_values(own_key, shape, scale, most, shards=(), kind=jnp.bfloat16):
    result = scale * jax.random.normal(own_key, shape, jnp.float32)
    if shards:
        result = result * levels(own_key, shape, shards, -0.22, 0.18)
    return jnp.clip(result, -most, most).astype(kind)


def setup_inputs(seed: int = 0) -> dict:
    arg_keys = jax.random.split(jax.random.key(seed), 8)
    tokens = draw_tokens(jax.random.fold_in(arg_keys[7], 71), 0)
    norm_gain = jnp.clip(1.0 + 0.18 * jax.random.normal(arg_keys[1], (D,), jnp.float32), 0.099609375, 1.8984375).astype(jnp.bfloat16)
    expert_ids_keys = jax.random.split(jax.random.fold_in(arg_keys[2], 1), TOKENS // TOK_DEV)
    expert_ids_turns = jax.random.permutation(jax.random.fold_in(arg_keys[2], 3), TOKENS // TOK_DEV)
    expert_ids = jax.vmap(lambda own, number: routed_block(jax.random.fold_in(arg_keys[2], 2), own, number, TOK_DEV, EXPERTS, 2, CAP, 2))(expert_ids_keys, expert_ids_turns).reshape((TOKENS, 2))
    gate_share = jnp.clip(0.1 + 0.9 * jax.random.uniform(arg_keys[3], (TOKENS, 2), jnp.float32) ** levels(arg_keys[3], (TOKENS, 2), ((0, 8),), -0.2, 0.2), 0.1, 1.0)
    gate_weight = normal_values(arg_keys[4], (EXPERTS, D, FF), D ** -0.5, 0.125, ((0, 8), (2, 4)))
    up_weight = normal_values(arg_keys[5], (EXPERTS, D, FF), D ** -0.5, 0.125, ((0, 8), (2, 4)))
    down_weight = normal_values(arg_keys[6], (EXPERTS, FF, D), FF ** -0.5, 0.09375, ((0, 8), (1, 4)))
    return {"tokens": tokens, "norm_gain": norm_gain, "expert_ids": expert_ids, "gate_share": gate_share, "gate_weight": gate_weight, "up_weight": up_weight, "down_weight": down_weight}


EPS = 1e-06

def reference(tokens, norm_gain, expert_ids, gate_share, gate_weight, up_weight, down_weight):
    xf = tokens.astype(jnp.float32)
    factor = lax.rsqrt(lax.optimization_barrier(jnp.mean(xf * xf, axis=1, keepdims=True)) + EPS)
    normed = (xf * factor * norm_gain.astype(jnp.float32)[None, :]).astype(jnp.bfloat16)
    blocks = expert_ids.reshape(N_EP, TOK_DEV * 2)
    onehot = (blocks[:, :, None] == jnp.arange(EXPERTS, dtype=jnp.int32)[None, None, :]).astype(jnp.int32)
    slots = lax.optimization_barrier(jnp.sum((jnp.cumsum(onehot, axis=1) - onehot) * onehot, axis=2))
    source = jnp.arange(N_EP, dtype=jnp.int32)[:, None]
    position = (source * CAP + slots).reshape(-1).astype(jnp.int32)
    flat_ids = expert_ids.reshape(-1).astype(jnp.int32)
    rows = jnp.repeat(normed, 2, axis=0)
    buffer = jnp.zeros((EXPERTS, N_EP * CAP, D), jnp.bfloat16).at[flat_ids, position].set(rows)
    width = FF // N_TP

    def expert(args):
        buf, w_gate, w_up, w_down = args
        gate = jnp.dot(buf, w_gate, preferred_element_type=jnp.float32)
        upper = jnp.dot(buf, w_up, preferred_element_type=jnp.float32)
        hidden = (jax.nn.silu(gate) * upper).astype(jnp.bfloat16)

        def add_block(index, total):
            piece = lax.dynamic_slice_in_dim(hidden, index * width, width, 1)
            wpiece = lax.dynamic_slice_in_dim(w_down, index * width, width, 0)
            term = jnp.dot(piece, wpiece, preferred_element_type=jnp.float32).astype(jnp.bfloat16)
            return total + lax.optimization_barrier(term).astype(jnp.float32)
        total = lax.fori_loop(0, N_TP, add_block, jnp.zeros((buf.shape[0], D), jnp.float32))
        return total.astype(jnp.bfloat16)
    outputs = lax.map(expert, (buffer, gate_weight, up_weight, down_weight))
    picked = outputs[flat_ids, position].astype(jnp.float32).reshape(TOKENS, 2, D)
    return lax.optimization_barrier(jnp.sum(picked * gate_share[:, :, None], axis=1)).astype(jnp.bfloat16)
```

```python
import functools
import jax
import jax.numpy as jnp
from jax import lax
from jax.experimental import pallas as pl
from jax.experimental.pallas import tpu as pltpu
from jax.sharding import PartitionSpec as P

D = 2048


EPS = 1e-06
MESH = pl.DeviceIdType.MESH
BF = jnp.bfloat16
F32 = jnp.float32
CORES = 2


def plain(tokens, norm_gain, expert_ids, gate_share, gate_weight, up_weight, down_weight):
    n_expdev = lax.axis_size("ep")
    exp_local = gate_weight.shape[0]
    experts = exp_local * n_expdev
    tok_rows = tokens.shape[0]
    slot_cap = 4 * tok_rows // experts
    flat_ids = expert_ids.reshape(-1)
    onehot = (flat_ids[:, None] == jnp.arange(experts, dtype=jnp.int32)[None, :]).astype(jnp.int32)
    slots = jnp.sum((jnp.cumsum(onehot, axis=0) - onehot) * onehot, axis=1)
    target = flat_ids * slot_cap + slots
    values = tokens.astype(jnp.float32)
    squares = lax.psum(jnp.sum(values * values, axis=1), "tp")
    factor = lax.rsqrt(squares / D + EPS)
    normed = (values * factor[:, None] * norm_gain.astype(jnp.float32)[None, :]).astype(
        jnp.bfloat16
    )
    rows = jnp.repeat(normed, 2, axis=0)
    buffer = jnp.zeros((experts * slot_cap, normed.shape[1]), jnp.bfloat16).at[target].set(rows)
    buffer = buffer.reshape(n_expdev, exp_local, slot_cap, normed.shape[1])
    arrived = lax.all_to_all(buffer, "ep", split_axis=0, concat_axis=0, tiled=True)
    piece = lax.all_gather(arrived, "tp", axis=3, tiled=True)
    first = jnp.einsum("secd,edf->secf", piece, gate_weight, preferred_element_type=jnp.float32)
    second = jnp.einsum("secd,edf->secf", piece, up_weight, preferred_element_type=jnp.float32)
    hidden = (jax.nn.silu(first) * second).astype(jnp.bfloat16)
    width_local = D // lax.axis_size("tp")
    term = jnp.einsum("secf,efd->dsec", hidden, down_weight, preferred_element_type=jnp.float32)
    summed = lax.psum_scatter(
        term.reshape(lax.axis_size("tp") * width_local, n_expdev * exp_local * slot_cap).astype(
            jnp.bfloat16
        ),
        "tp",
        scatter_dimension=0,
        tiled=True,
    )
    results = summed.reshape(width_local, n_expdev, exp_local, slot_cap)
    results = jnp.transpose(results, (1, 2, 3, 0))
    returned = lax.all_to_all(results, "ep", split_axis=0, concat_axis=0, tiled=True)
    flat_back = returned.reshape(experts * slot_cap, width_local)
    picked = flat_back[target].astype(jnp.float32).reshape(tok_rows, 2, width_local)
    return jnp.sum(picked * gate_share[:, :, None], axis=1).astype(jnp.bfloat16)


def fused(
    n, n_tp, early,
    tok_ref, gain_ref, ids_ref, share_ref, wg_hbm, wu_hbm, wd_hbm,
    out_ref,
    wg, wu, wd, part, near, far, slot_row, share_row, send_a, send_b, xs,
    hid, own_y, ys, yd, za, zs, zx, rs, ra, mix_hi, mix_lo,
    w_sem, p_send, p_recv, n_send, n_recv, a_send, a_recv, b_send, b_recv,
    d_send, d_recv, y_send, y_recv, z_send, z_recv, r_send, r_recv,
):
    me = lax.axis_index("ep")
    tp = lax.axis_index("tp")
    x, c = tp // CORES, tp % CORES
    partner = x * CORES + (1 - c)
    across = (1 - x) * CORES + c
    diag = (1 - x) * CORES + (1 - c)
    rows, width = tok_ref.shape
    cap = send_a.shape[1]

    loads = [
        pltpu.make_async_copy(wg_hbm.at[0], wg, w_sem.at[0]),
        pltpu.make_async_copy(wu_hbm.at[0], wu, w_sem.at[1]),
    ] + [
        pltpu.make_async_copy(wd_hbm.at[0, :, pl.ds(q * width, width)], wd.at[q], w_sem.at[2 + q])
        for q in range(n_tp)
    ]
    for load in loads:
        load.start()

    barrier = pltpu.get_barrier_semaphore()
    for other in (partner, across, diag):
        pl.semaphore_signal(barrier, inc=1, device_id=(me, other), device_id_type=MESH)
    for k in range(1, n):
        pl.semaphore_signal(barrier, inc=1, device_id=((me + k) % n, tp), device_id_type=MESH)

    def remote(src, dst, ssem, rsem, e, t):
        return pltpu.make_async_remote_copy(
            src_ref=src, dst_ref=dst, send_sem=ssem, recv_sem=rsem,
            device_id=(e, t), device_id_type=MESH,
        )

    def lanes_to_rows(v):
        return jnp.transpose(v)

    xf = tok_ref[...].astype(F32)
    sq = xf * xf
    groups = sq[:, 0:128]
    for j in range(1, width // 128):
        groups = groups + sq[:, j * 128:(j + 1) * 128]
    mine = jnp.sum(lanes_to_rows(groups), axis=0, keepdims=True)
    part[0] = jnp.broadcast_to(mine, (8, rows))

    pl.semaphore_wait(barrier, 3 + n - 1)
    p_copies = [
        remote(part.at[0], part.at[j], p_send.at[j], p_recv.at[j], me, other)
        for j, other in ((1, partner), (2, across), (3, diag))
    ]
    for copy in p_copies:
        copy.start()

    experts = slot_row.shape[0]
    expert_of = lax.broadcasted_iota(jnp.int32, (experts, rows), 0)
    first = expert_of == ids_ref[0:1, :]
    second = expert_of == ids_ref[1:2, :]
    named = jnp.where(first | second, 1.0, 0.0)
    before = (
        lax.broadcasted_iota(jnp.int32, (rows, rows), 0)
        < lax.broadcasted_iota(jnp.int32, (rows, rows), 1)
    )
    earlier = jnp.dot(
        named.astype(BF), jnp.where(before, 1.0, 0.0).astype(BF), preferred_element_type=F32
    )
    slot_row[...] = jnp.where(named > 0.5, earlier, -1.0)
    share_row[...] = jnp.where(first, share_ref[0:1, :], 0.0) + jnp.where(
        second, share_ref[1:2, :], 0.0
    )
    slot_of = lax.broadcasted_iota(jnp.int32, (cap, rows), 0).astype(F32)

    def placed(k):
        e = (me + k) % n
        return slot_of == jnp.broadcast_to(slot_row[pl.ds(e, 1), :], (cap, rows))

    def place(k):
        return jnp.where(placed(k), 1.0, 0.0).astype(BF)

    for copy in p_copies:
        copy.wait_recv()
    total = part[0] + part[1] + part[2] + part[3]
    factor = lax.rsqrt(total[0:1, :] / (width * n_tp) + EPS)
    column = jnp.transpose(jnp.broadcast_to(factor, (128, rows)))
    column = jnp.concatenate([column] * (width // 128), axis=1)
    near[...] = (xf * column * gain_ref[...].astype(F32)).astype(BF)
    n_copy = remote(near, far, n_send, n_recv, me, across)
    n_copy.start()

    def a_copy(k, e):
        return remote(send_a.at[k], xs.at[k, c, x], a_send.at[k], a_recv.at[k], e, tp)

    def b_copy(k, e):
        return remote(send_b.at[k], xs.at[k, c, 1 - x], b_send.at[k], b_recv.at[k], e, tp)

    def send_near(k):
        send_a[k] = jnp.dot(place(k), near[...], preferred_element_type=F32).astype(BF)
        a_copy(k, (me + k) % n).start()

    def send_far(k):
        send_b[k] = jnp.dot(place(k), far[...], preferred_element_type=F32).astype(BF)
        b_copy(k, (me + k) % n).start()

    @pl.loop(1, early)
    def _(k):
        send_near(k)

    xs[0, c, x] = jnp.dot(place(0), near[...], preferred_element_type=F32).astype(BF)

    def weigh(k):
        e = (me + k) % n
        weight = jnp.where(
            placed(k), jnp.broadcast_to(share_row[pl.ds(e, 1), :], (cap, rows)), 0.0
        )
        weight = jnp.transpose(weight)
        high = weight.astype(BF)
        mix_hi[k] = high
        mix_lo[k] = (weight - high.astype(F32)).astype(BF)

    n_copy.wait_recv()
    xs[0, c, 1 - x] = jnp.dot(place(0), far[...], preferred_element_type=F32).astype(BF)

    def d_copy(k):
        return remote(xs.at[k, c], xs.at[k, c], d_send.at[k], d_recv.at[k], me, partner)

    def d_arrival(k):
        return remote(xs.at[k, 1 - c], xs.at[k, 1 - c], d_send.at[k], d_recv.at[k], me, partner)

    def y_copy(k):
        return remote(ys.at[k], yd.at[k], y_send.at[k], y_recv.at[k], me, partner)

    def z_copy(k):
        return remote(zs.at[k], zx.at[k], z_send.at[k], z_recv.at[k], me, across)

    def r_copy(k):
        return remote(rs.at[k], ra.at[k], r_send.at[k], r_recv.at[k], (me + n - k) % n, tp)

    @pl.loop(1, early)
    def _(k):
        send_far(k)

    @pl.loop(early, n)
    def _(k):
        send_near(k)
        send_far(k)

    @pl.loop(0, n)
    def _(k):
        weigh(k)

    for load in loads:
        load.wait()

    def column_of(q_x, q_c):
        return wd[q_x * CORES + q_c]

    ff = wg.shape[1]
    tile = 256 if ff % 256 == 0 else 128

    @pl.loop(0, n + 2)
    def _(k):
        @pl.when((k >= 1) & (k < n))
        def _():
            a_copy(k, me).wait_recv()
            b_copy(k, me).wait_recv()

        @pl.when(k < n)
        def _():
            d_copy(k).start()

        @pl.when((k >= 1) & (k <= n))
        def _():
            j = k - 1
            y_copy(j).wait_recv()
            zs[j] = (own_y[j, 1] + yd[j, 1].astype(F32)).astype(BF)
            z_copy(j).start()
            za[j] = own_y[j, 0] + yd[j, 0].astype(F32)

        @pl.when(k < n)
        def _():
            d_arrival(k).wait_recv()
            block = jnp.concatenate(
                [xs[k, q % CORES, q // CORES] for q in range(n_tp)], axis=1
            )
            for f in range(0, ff, tile):
                gate = jnp.dot(block, wg[:, f:f + tile], preferred_element_type=F32)
                up = jnp.dot(block, wu[:, f:f + tile], preferred_element_type=F32)
                hid[:, f:f + tile] = (gate / (1.0 + jnp.exp(-gate)) * up).astype(BF)
            hidden = hid[...]
            for i, q_x in enumerate((x, 1 - x)):
                ys[k, i] = jnp.dot(
                    hidden, column_of(q_x, 1 - c), preferred_element_type=F32
                ).astype(BF)
            y_copy(k).start()
            for i, q_x in enumerate((x, 1 - x)):
                own_y[k, i] = jnp.dot(hidden, column_of(q_x, c), preferred_element_type=F32)

        @pl.when(k >= 2)
        def _():
            j = k - 2
            z_copy(j).wait_recv()
            result = (za[j] + zx[j].astype(F32)).astype(BF)

            @pl.when(j == 0)
            def _():
                ra[0] = result

            @pl.when(j > 0)
            def _():
                rs[j] = result
                r_copy(j).start()

    def mixed(k):
        back = ra[k]
        return jnp.dot(mix_hi[k], back, preferred_element_type=F32) + jnp.dot(
            mix_lo[k], back, preferred_element_type=F32
        )

    total = mixed(0)
    for k in range(1, n):
        r_copy(k).wait_recv()
        total = total + mixed(k)
    out_ref[...] = total.astype(BF)

    for copy in p_copies:
        copy.wait_send()
    n_copy.wait_send()
    for k in range(n):
        d_copy(k).wait_send()
        y_copy(k).wait_send()
        z_copy(k).wait_send()
        if k:
            a_copy(k, me).wait_send()
            b_copy(k, me).wait_send()
            r_copy(k).wait_send()


def routed(n, n_tp, tokens, norm_gain, expert_ids, gate_share, gate_weight, up_weight, down_weight):
    rows, width = tokens.shape
    experts = n * gate_weight.shape[0]
    cap = 4 * rows // experts
    depth, ff = gate_weight.shape[1:]
    vmem = pl.BlockSpec(memory_space=pltpu.VMEM)
    hbm = pl.BlockSpec(memory_space=pltpu.HBM)
    dma = pltpu.SemaphoreType.DMA
    return pl.pallas_call(
        functools.partial(fused, n, n_tp, (n + 1) // 2),
        out_shape=jax.ShapeDtypeStruct((rows, width), BF),
        in_specs=[vmem] * 4 + [hbm] * 3,
        out_specs=vmem,
        scratch_shapes=[
            pltpu.VMEM((depth, ff), BF),
            pltpu.VMEM((depth, ff), BF),
            pltpu.VMEM((n_tp, ff, width), BF),
            pltpu.VMEM((4, 8, rows), F32),
            pltpu.VMEM((rows, width), BF),
            pltpu.VMEM((rows, width), BF),
            pltpu.VMEM((experts, rows), F32),
            pltpu.VMEM((experts, rows), F32),
            pltpu.VMEM((n, cap, width), BF),
            pltpu.VMEM((n, cap, width), BF),
            pltpu.VMEM((n, CORES, n_tp // CORES, cap, width), BF),
            pltpu.VMEM((cap, ff), BF),
            pltpu.VMEM((n, 2, cap, width), F32),
            pltpu.VMEM((n, 2, cap, width), BF),
            pltpu.VMEM((n, 2, cap, width), BF),
            pltpu.VMEM((n, cap, width), F32),
            pltpu.VMEM((n, cap, width), BF),
            pltpu.VMEM((n, cap, width), BF),
            pltpu.VMEM((n, cap, width), BF),
            pltpu.VMEM((n, cap, width), BF),
            pltpu.VMEM((n, rows, cap), BF),
            pltpu.VMEM((n, rows, cap), BF),
            dma((2 + n_tp,)),
            dma((4,)), dma((4,)),
            dma, dma,
            dma((n,)), dma((n,)),
            dma((n,)), dma((n,)),
            dma((n,)), dma((n,)),
            dma((n,)), dma((n,)),
            dma((n,)), dma((n,)),
            dma((n,)), dma((n,)),
        ],
        compiler_params=pltpu.CompilerParams(
            collective_id=0, has_side_effects=True, vmem_limit_bytes=56 * 1024 * 1024
        ),
    )(
        tokens, norm_gain.reshape(1, width), expert_ids.T, gate_share.T,
        gate_weight, up_weight, down_weight,
    )


def shards(n, n_tp, *args):
    tokens, gate_weight = args[0], args[4]
    rows, width = tokens.shape
    cap = 4 * rows // (n * gate_weight.shape[0])
    fits = (
        n_tp == 2 * CORES and gate_weight.shape[0] == 1 and rows % 128 == 0
        and width % 128 == 0 and gate_weight.shape[2] % 128 == 0 and cap % 128 == 0
    )
    return routed(n, n_tp, *args) if fits else plain(*args)


def solution(mesh):
    body = functools.partial(shards, mesh.shape["ep"], mesh.shape["tp"])
    in_specs = (
        P("ep", "tp"),
        P("tp"),
        P("ep", None),
        P("ep", None),
        P("ep", None, "tp"),
        P("ep", None, "tp"),
        P("ep", "tp", None),
    )
    out_specs = P("ep", "tp")
    return jax.shard_map(body, mesh=mesh, in_specs=in_specs, out_specs=out_specs, check_vma=False)
```

```python
import functools
import jax
import jax.numpy as jnp
from jax import lax
from jax.experimental import pallas as pl
from jax.experimental.pallas import tpu as pltpu
from jax.sharding import PartitionSpec as P

D = 2048


EPS = 1e-06
MESH = pl.DeviceIdType.MESH
BF = jnp.bfloat16
F32 = jnp.float32
CORES = 2


def plain(tokens, norm_gain, expert_ids, gate_share, gate_weight, up_weight, down_weight):
    n_expdev = lax.axis_size("ep")
    exp_local = gate_weight.shape[0]
    experts = exp_local * n_expdev
    tok_rows = tokens.shape[0]
    slot_cap = 4 * tok_rows // experts
    flat_ids = expert_ids.reshape(-1)
    onehot = (flat_ids[:, None] == jnp.arange(experts, dtype=jnp.int32)[None, :]).astype(jnp.int32)
    slots = jnp.sum((jnp.cumsum(onehot, axis=0) - onehot) * onehot, axis=1)
    target = flat_ids * slot_cap + slots
    values = tokens.astype(jnp.float32)
    squares = lax.psum(jnp.sum(values * values, axis=1), "tp")
    factor = lax.rsqrt(squares / D + EPS)
    normed = (values * factor[:, None] * norm_gain.astype(jnp.float32)[None, :]).astype(
        jnp.bfloat16
    )
    rows = jnp.repeat(normed, 2, axis=0)
    buffer = jnp.zeros((experts * slot_cap, normed.shape[1]), jnp.bfloat16).at[target].set(rows)
    buffer = buffer.reshape(n_expdev, exp_local, slot_cap, normed.shape[1])
    arrived = lax.all_to_all(buffer, "ep", split_axis=0, concat_axis=0, tiled=True)
    piece = lax.all_gather(arrived, "tp", axis=3, tiled=True)
    first = jnp.einsum("secd,edf->secf", piece, gate_weight, preferred_element_type=jnp.float32)
    second = jnp.einsum("secd,edf->secf", piece, up_weight, preferred_element_type=jnp.float32)
    hidden = (jax.nn.silu(first) * second).astype(jnp.bfloat16)
    width_local = D // lax.axis_size("tp")
    term = jnp.einsum("secf,efd->dsec", hidden, down_weight, preferred_element_type=jnp.float32)
    summed = lax.psum_scatter(
        term.reshape(lax.axis_size("tp") * width_local, n_expdev * exp_local * slot_cap).astype(
            jnp.bfloat16
        ),
        "tp",
        scatter_dimension=0,
        tiled=True,
    )
    results = summed.reshape(width_local, n_expdev, exp_local, slot_cap)
    results = jnp.transpose(results, (1, 2, 3, 0))
    returned = lax.all_to_all(results, "ep", split_axis=0, concat_axis=0, tiled=True)
    flat_back = returned.reshape(experts * slot_cap, width_local)
    picked = flat_back[target].astype(jnp.float32).reshape(tok_rows, 2, width_local)
    return jnp.sum(picked * gate_share[:, :, None], axis=1).astype(jnp.bfloat16)


def fused(
    n, n_tp, steps,
    tok_ref, gain_ref, ids_ref, share_ref, wg_hbm, wu_hbm, wd_hbm,
    out_ref,
    wg, wu, wd, part, near, far, slot_row, share_row, send_a, send_b, xs,
    hid, own_y, ys, yd, za, zs, zx, rs, ra, mix_hi, mix_lo,
    w_sem, p_send, p_recv, n_send, n_recv, a_send, a_recv, b_send, b_recv,
    f_send, f_recv, d_send, d_recv, e_send, e_recv, y_send, y_recv, z_send, z_recv, r_send, r_recv,
):
    me = lax.axis_index("ep")
    tp = lax.axis_index("tp")
    x, c = tp // CORES, tp % CORES
    partner = x * CORES + (1 - c)
    across = (1 - x) * CORES + c
    diag = (1 - x) * CORES + (1 - c)
    rows, width = tok_ref.shape
    cap = send_a.shape[1]
    half = n // 2

    def peer(k):
        found, bit = 0, 1
        while bit < n:
            found = found + (me // bit + k // bit) % 2 * bit
            bit *= 2
        return found

    loads = [
        pltpu.make_async_copy(wg_hbm.at[0], wg, w_sem.at[0]),
        pltpu.make_async_copy(wu_hbm.at[0], wu, w_sem.at[1]),
    ] + [
        pltpu.make_async_copy(wd_hbm.at[0, :, pl.ds(q * width, width)], wd.at[q], w_sem.at[2 + q])
        for q in range(n_tp)
    ]
    for load in loads:
        load.start()

    barrier = pltpu.get_barrier_semaphore()
    for other in (partner, across, diag):
        pl.semaphore_signal(barrier, inc=1, device_id=(me, other), device_id_type=MESH)
    for k in range(1, n):
        pl.semaphore_signal(barrier, inc=1, device_id=(peer(k), tp), device_id_type=MESH)

    def remote(src, dst, ssem, rsem, e, t):
        return pltpu.make_async_remote_copy(
            src_ref=src, dst_ref=dst, send_sem=ssem, recv_sem=rsem,
            device_id=(e, t), device_id_type=MESH,
        )

    def lanes_to_rows(v):
        return jnp.transpose(v)

    xf = tok_ref[...].astype(F32)
    sq = xf * xf
    groups = sq[:, 0:128]
    for j in range(1, width // 128):
        groups = groups + sq[:, j * 128:(j + 1) * 128]
    mine = jnp.sum(lanes_to_rows(groups), axis=0, keepdims=True)
    part[0] = jnp.broadcast_to(mine, (8, rows))

    pl.semaphore_wait(barrier, 3 + n - 1)
    p_copies = [
        remote(part.at[0], part.at[j], p_send.at[j], p_recv.at[j], me, other)
        for j, other in ((1, partner), (2, across), (3, diag))
    ]
    for copy in p_copies:
        copy.start()

    experts = slot_row.shape[0]
    expert_of = lax.broadcasted_iota(jnp.int32, (experts, rows), 0)
    first = expert_of == ids_ref[0:1, :]
    second = expert_of == ids_ref[1:2, :]
    named = jnp.where(first | second, 1.0, 0.0)
    before = (
        lax.broadcasted_iota(jnp.int32, (rows, rows), 0)
        < lax.broadcasted_iota(jnp.int32, (rows, rows), 1)
    )
    earlier = jnp.dot(
        named.astype(BF), jnp.where(before, 1.0, 0.0).astype(BF), preferred_element_type=F32
    )
    slot_row[...] = jnp.where(named > 0.5, earlier, -1.0)
    share_row[...] = jnp.where(first, share_ref[0:1, :], 0.0) + jnp.where(
        second, share_ref[1:2, :], 0.0
    )
    slot_of = lax.broadcasted_iota(jnp.int32, (cap, rows), 0).astype(F32)

    def placed(k):
        e = peer(k)
        return slot_of == jnp.broadcast_to(slot_row[pl.ds(e, 1), :], (cap, rows))

    def place(k):
        return jnp.where(placed(k), 1.0, 0.0).astype(BF)

    for copy in p_copies:
        copy.wait_recv()
    total = part[0] + part[1] + part[2] + part[3]
    factor = lax.rsqrt(total[0:1, :] / (width * n_tp) + EPS)
    column = jnp.transpose(jnp.broadcast_to(factor, (128, rows)))
    column = jnp.concatenate([column] * (width // 128), axis=1)
    near[...] = (xf * column * gain_ref[...].astype(F32)).astype(BF)
    n_copy = remote(near, far, n_send, n_recv, me, across)
    n_copy.start()

    def a_copy(k, e):
        return remote(send_a.at[k], xs.at[k, c, x], a_send.at[k], a_recv.at[k], e, tp)

    def b_copy(k, e):
        return remote(send_b.at[k], xs.at[k, c, 1 - x], b_send.at[k], b_recv.at[k], e, tp)

    def send_near(k):
        send_a[k] = jnp.dot(place(k), near[...], preferred_element_type=F32).astype(BF)
        a_copy(k, peer(k)).start()

    def send_far(k):
        send_b[k] = jnp.dot(place(k), far[...], preferred_element_type=F32).astype(BF)
        b_copy(k, peer(k)).start()

    first_far = half + half // 2
    for k in range(half, first_far):
        send_near(k)
    for k in range(1, half):
        send_near(k)

    xs[0, c, x] = jnp.dot(place(0), near[...], preferred_element_type=F32).astype(BF)

    def weigh(k):
        e = peer(k)
        weight = jnp.where(
            placed(k), jnp.broadcast_to(share_row[pl.ds(e, 1), :], (cap, rows)), 0.0
        )
        weight = jnp.transpose(weight)
        high = weight.astype(BF)
        mix_hi[k] = high
        mix_lo[k] = (weight - high.astype(F32)).astype(BF)

    n_copy.wait_recv()
    xs[0, c, 1 - x] = jnp.dot(place(0), far[...], preferred_element_type=F32).astype(BF)

    for i in range(max(half - 1, n - first_far)):
        if i + 1 < half:
            send_far(i + 1)
        if first_far + i < n:
            send_near(first_far + i)

    def f_copy(k):
        return remote(xs.at[k, c, x], xs.at[k, c, x], f_send.at[k], f_recv.at[k], me, across)

    def f_arrival(k):
        there = xs.at[k, c, 1 - x]
        return remote(there, there, f_send.at[k], f_recv.at[k], me, across)

    def d_copy(k, core):
        ref = xs.at[k, core] if k < half else xs.at[k, core, x]
        return remote(ref, ref, d_send.at[k], d_recv.at[k], me, partner)

    def e_copy(k, core):
        ref = xs.at[k, core, 1 - x]
        return remote(ref, ref, e_send.at[k], e_recv.at[k], me, partner)

    def y_copy(k):
        return remote(ys.at[k], yd.at[k], y_send.at[k], y_recv.at[k], me, partner)

    def z_copy(k):
        return remote(zs.at[k], zx.at[k], z_send.at[k], z_recv.at[k], me, across)

    def r_copy(k):
        return remote(rs.at[k], ra.at[k], r_send.at[k], r_recv.at[k], peer(k), tp)

    def arrive(ks):
        for k in ks:
            if k:
                a_copy(k, me).wait_recv()
            if k >= half:
                f_copy(k).start()
            elif k:
                b_copy(k, me).wait_recv()
            d_copy(k, c).start()

    def pair(ks):
        for k in ks:
            y_copy(k).wait_recv()
            zs[k] = (own_y[k, 1] + yd[k, 1].astype(F32)).astype(BF)
            z_copy(k).start()
        for k in ks:
            za[k] = own_y[k, 0] + yd[k, 0].astype(F32)

    def give(ks):
        for k in ks:
            z_copy(k).wait_recv()
            result = (za[k] + zx[k].astype(F32)).astype(BF)
            if k:
                rs[k] = result
                r_copy(k).start()
            else:
                ra[0] = result

    ff = wg.shape[1]
    tile = 256 if ff % 256 == 0 else 128

    arrive(steps[0])

    @pl.loop(0, n)
    def _(k):
        weigh(k)

    for load in loads:
        load.wait()

    for step, ks in enumerate(steps):
        for k in ks:
            if k >= half:
                f_arrival(k).wait_recv()
                e_copy(k, c).start()
        if step >= 1:
            pair(steps[step - 1])
        if step >= 2:
            give(steps[step - 2])
        for k in ks:
            d_copy(k, 1 - c).wait_recv()
            if k >= half:
                e_copy(k, 1 - c).wait_recv()
        block = jnp.concatenate(
            [
                jnp.concatenate([xs[k, q % CORES, q // CORES] for q in range(n_tp)], axis=1)
                for k in ks
            ],
            axis=0,
        )
        held = cap * len(ks)
        for f in range(0, ff, tile):
            gate = jnp.dot(block, wg[:, f:f + tile], preferred_element_type=F32)
            up = jnp.dot(block, wu[:, f:f + tile], preferred_element_type=F32)
            hid[0:held, f:f + tile] = (gate / (1.0 + jnp.exp(-gate)) * up).astype(BF)
        if step + 1 < len(steps):
            arrive(steps[step + 1])
        hidden = hid[0:held, :]
        for i, q_x in enumerate((x, 1 - x)):
            y = jnp.dot(hidden, wd[q_x * CORES + 1 - c], preferred_element_type=F32).astype(BF)
            for m, k in enumerate(ks):
                ys[k, i] = y[m * cap:(m + 1) * cap]
        for k in ks:
            y_copy(k).start()
        for i, q_x in enumerate((x, 1 - x)):
            y = jnp.dot(hidden, wd[q_x * CORES + c], preferred_element_type=F32)
            for m, k in enumerate(ks):
                own_y[k, i] = y[m * cap:(m + 1) * cap]
    pair(steps[-1])
    for ks in steps[-2:]:
        give(ks)

    def mixed(k):
        back = ra[k]
        return jnp.dot(mix_hi[k], back, preferred_element_type=F32) + jnp.dot(
            mix_lo[k], back, preferred_element_type=F32
        )

    total = mixed(0)
    for k in [k for ks in steps for k in ks if k]:
        r_copy(k).wait_recv()
        total = total + mixed(k)
    out_ref[...] = total.astype(BF)

    for copy in p_copies:
        copy.wait_send()
    n_copy.wait_send()
    for k in range(n):
        d_copy(k, c).wait_send()
        y_copy(k).wait_send()
        z_copy(k).wait_send()
        if k:
            a_copy(k, me).wait_send()
            r_copy(k).wait_send()
        if 0 < k < half:
            b_copy(k, me).wait_send()
        if k >= half:
            f_copy(k).wait_send()
            e_copy(k, c).wait_send()


def order(n):
    half, quarter = n // 2, n // 4
    starts = (0, half, quarter, half + quarter)
    return [tuple(range(i, i + 2)) for s in starts for i in range(s, s + quarter, 2)]


def routed(n, n_tp, tokens, norm_gain, expert_ids, gate_share, gate_weight, up_weight, down_weight):
    rows, width = tokens.shape
    experts = n * gate_weight.shape[0]
    cap = 4 * rows // experts
    depth, ff = gate_weight.shape[1:]
    vmem = pl.BlockSpec(memory_space=pltpu.VMEM)
    hbm = pl.BlockSpec(memory_space=pltpu.HBM)
    dma = pltpu.SemaphoreType.DMA
    return pl.pallas_call(
        functools.partial(fused, n, n_tp, order(n)),
        out_shape=jax.ShapeDtypeStruct((rows, width), BF),
        in_specs=[vmem] * 4 + [hbm] * 3,
        out_specs=vmem,
        scratch_shapes=[
            pltpu.VMEM((depth, ff), BF),
            pltpu.VMEM((depth, ff), BF),
            pltpu.VMEM((n_tp, ff, width), BF),
            pltpu.VMEM((4, 8, rows), F32),
            pltpu.VMEM((rows, width), BF),
            pltpu.VMEM((rows, width), BF),
            pltpu.VMEM((experts, rows), F32),
            pltpu.VMEM((experts, rows), F32),
            pltpu.VMEM((n, cap, width), BF),
            pltpu.VMEM((n, cap, width), BF),
            pltpu.VMEM((n, CORES, n_tp // CORES, cap, width), BF),
            pltpu.VMEM((2 * cap, ff), BF),
            pltpu.VMEM((n, 2, cap, width), F32),
            pltpu.VMEM((n, 2, cap, width), BF),
            pltpu.VMEM((n, 2, cap, width), BF),
            pltpu.VMEM((n, cap, width), F32),
            pltpu.VMEM((n, cap, width), BF),
            pltpu.VMEM((n, cap, width), BF),
            pltpu.VMEM((n, cap, width), BF),
            pltpu.VMEM((n, cap, width), BF),
            pltpu.VMEM((n, rows, cap), BF),
            pltpu.VMEM((n, rows, cap), BF),
            dma((2 + n_tp,)),
            dma((4,)), dma((4,)),
            dma, dma,
            dma((n,)), dma((n,)),
            dma((n,)), dma((n,)),
            dma((n,)), dma((n,)),
            dma((n,)), dma((n,)),
            dma((n,)), dma((n,)),
            dma((n,)), dma((n,)),
            dma((n,)), dma((n,)),
            dma((n,)), dma((n,)),
        ],
        compiler_params=pltpu.CompilerParams(
            collective_id=0, has_side_effects=True, vmem_limit_bytes=56 * 1024 * 1024
        ),
    )(
        tokens, norm_gain.reshape(1, width), expert_ids.T, gate_share.T,
        gate_weight, up_weight, down_weight,
    )


def shards(n, n_tp, *args):
    tokens, gate_weight = args[0], args[4]
    rows, width = tokens.shape
    cap = 4 * rows // (n * gate_weight.shape[0])
    fits = (
        n_tp == 2 * CORES and n >= 8 and n & (n - 1) == 0 and gate_weight.shape[0] == 1 and rows % 128 == 0
        and width % 128 == 0 and gate_weight.shape[2] % 128 == 0 and cap % 128 == 0
    )
    return routed(n, n_tp, *args) if fits else plain(*args)


def solution(mesh):
    body = functools.partial(shards, mesh.shape["ep"], mesh.shape["tp"])
    in_specs = (
        P("ep", "tp"),
        P("tp"),
        P("ep", None),
        P("ep", None),
        P("ep", None, "tp"),
        P("ep", None, "tp"),
        P("ep", "tp", None),
    )
    out_specs = P("ep", "tp")
    return jax.shard_map(body, mesh=mesh, in_specs=in_specs, out_specs=out_specs, check_vma=False)
```
